32 devices in a mesh: grp: 2 (over x), ep: 8 (over z, y), tp: 2 (over core).
Axes of the slice: x: 2, y: 2, z: 4, core: 2. Of those that a mesh axis runs over, the one named last changes fastest.
Arguments:
- tokens: bfloat16 [8192, 2048], P(('grp', 'ep', 'tp')), parts along dimension 0, may hold values from -6 to 6
- norm_gain: float32 [2048], replicated, may hold values from 0.1 to 1.9
- expert_ids: int32 [8192, 4], P(('grp', 'ep', 'tp')), parts along dimension 0, may hold values from 0 to 31, all different within a row; in each aligned block of 256 rows (0 to 255, 256 to 511, ...) at most 40 rows name the same one
- gate_weights: float32 [8192, 4], P(('grp', 'ep', 'tp')), parts along dimension 0, may hold values from 0.1 to 1
- expert_gate: bfloat16 [32, 2048, 512], P('ep', None, 'tp'), may hold values from -0.125 to 0.125
- expert_up: bfloat16 [32, 2048, 512], P('ep', None, 'tp'), may hold values from -0.125 to 0.125
- expert_down: bfloat16 [32, 512, 2048], P('ep', 'tp'), may hold values from -0.25 to 0.25
- shared_gate: bfloat16 [2048, 512], replicated, may hold values from -0.125 to 0.125
- shared_up: bfloat16 [2048, 512], replicated, may hold values from -0.125 to 0.125
- shared_down: bfloat16 [512, 2048], replicated, may hold values from -0.25 to 0.25
- post_gain: float32 [2048], replicated, may hold values from 0.1 to 1.9
Outputs:
- mixed: bfloat16 [8192, 2048], P(('grp', 'ep', 'tp')), parts along dimension 0
The draws below stay inside these ranges and needn't reach their ends.
There are 2 independent parts, one for each index of `grp`. The reference program is written for one: setup_inputs(seed, part) draws one part's arguments, and reference() takes and returns one part's arrays. A program takes and returns all parts, laid end to end along the dimension named above; an argument that names none is the same for every part. Nothing has to cross between parts.
Inputs may be any that keep to these rules, and one draw needn't show every extreme that they name: `expert_ids`: each row names 4 different experts; in each device's aligned block of 256 rows no expert is named by more than 40 rows, a bound that some block reaches.
All inputs are finite; a program needn't handle non-finite values.
Results may differ from the reference program's by a relative error of at most 0.0067.
Values may be sent and summed in bfloat16 or wider, within the bound.
A program may use at most 128 MiB of HBM per device.

```python
import math
import jax
import jax.numpy as jnp
import numpy as np
from jax import lax

D = 2048
FE = 512
FS = 512
EXPERTS = 32
TOP_K = 4
TOK_DEV = 256
CAP = 40
TOKENS = 4096


def shard_levels(stream_key, dims, split, low, top_value):
    def one(axis_at, blocks):
        heights = jax.random.uniform(jax.random.fold_in(jax.random.fold_in(stream_key, 6), axis_at), (blocks,), jnp.float32, low / len(split), top_value / len(split))
        return jnp.repeat(jnp.exp(heights), dims[axis_at] // blocks).reshape((-1,) + (1,) * (len(dims) - axis_at - 1))

    level = one(*split[0])
    for cut in split[1:]:
        level = level * one(*cut)
    return level


def assign_block(rng, own, number, rows, amount, top, limit, lean):
    sequence = jax.random.permutation(rng, amount)
    heavy_load, common = load_shares(amount, rows * top, limit, lean, True), load_shares(amount, rows * top, limit, lean, False)
    places = jnp.arange(amount)

    def named(sizes, offset_by):
        used = int((sizes > 0).sum())
        fixed = max(1, used // 4)
        moved = fixed + (places - fixed + offset_by * (used - fixed)) % max(1, amount - fixed)
        return jnp.zeros((amount,), jnp.int32).at[sequence[jnp.where(places < fixed, places, moved)]].set(jnp.asarray(sizes, jnp.int32))

    sizes = jnp.where(number % 4 == 0, named(heavy_load, number // 4), named(common, number - number // 4 - 1))
    mixed = jax.random.permutation(jax.random.fold_in(own, 3), amount)
    source_of, taker = mixed[0:amount // 2 * 2:2], mixed[1:amount // 2 * 2:2]
    margin = jnp.minimum(sizes[source_of] - 1, limit - sizes[taker]) // 2
    margin = jnp.where((source_of == sequence[0]) | (taker == sequence[0]) | (sizes[taker] == 0), 0, jnp.maximum(margin, 0))
    moved = jax.random.randint(jax.random.fold_in(own, 4), (amount // 2,), 0, 1 << 20) % (margin + 1)
    sizes = sizes.at[source_of].add(-moved).at[taker].add(moved)
    items = jnp.searchsorted(jnp.cumsum(sizes), jnp.arange(rows * top), side="right").astype(jnp.int32)
    table = items.reshape(top, rows).T
    table = table[jax.random.permutation(jax.random.fold_in(own, 1), rows)]
    offset_by = jax.random.randint(jax.random.fold_in(own, 2), (rows, 1), 0, top)
    return jnp.take_along_axis(table, (jnp.arange(top)[None, :] + offset_by) % top, axis=1)


def load_shares(number_of, total, bound, skew, full):
    weights = [(1 << 20) // math.isqrt(rank ** skew) + 1 for rank in range(1, number_of + 1)]
    largest = bound if full else min(bound, max(-(-total // number_of), total * weights[0] // sum(weights)))
    least = 1 if total - largest >= number_of - 1 else 0
    holding, rest = [largest] + [least] * (number_of - 1), total - largest - least * (number_of - 1)
    while rest > 0:
        free = [i for i in range(1, number_of) if holding[i] < largest] or [i for i in range(1, number_of) if holding[i] < bound]
        pool, left = sum([weights[i] for i in free]), rest
        for i in free:
            more = min(bound - holding[i], max(1, left * weights[i] // pool), rest)
            holding[i] = holding[i] + more
            rest = rest - more
    return np.array(holding)


def gaussian(own_key, dims, scale, reach, shards=(), kind=jnp.bfloat16):
    drawn = jax.random.normal(own_key, dims, jnp.float32) * scale
    if len(shards) > 0:
        drawn = shard_levels(own_key, dims, shards, -0.22, 0.18) * drawn
    return jnp.clip(drawn, min=-reach, max=reach).astype(kind)


def setup_inputs(seed: int = 0, part: int = 0) -> dict:
    streams_of = jax.random.split(jax.random.key(seed), 12)
    own_keys = jax.random.split(jax.random.fold_in(streams_of[11], part), 12)
    tokens = gaussian(own_keys[0], (TOKENS, D), 1.0, 6.0, ((0, 16),))
    norm_gain = jnp.clip(1.0 + 0.18 * jax.random.normal(streams_of[1], (D,), jnp.float32), 0.1, 1.9)
    expert_ids_keys = jax.random.split(jax.random.fold_in(own_keys[2], 1), TOKENS // TOK_DEV)
    expert_ids_turns = jax.random.permutation(jax.random.fold_in(own_keys[2], 3), TOKENS // TOK_DEV)
    expert_ids = jax.vmap(lambda own, number: assign_block(jax.random.fold_in(own_keys[2], 2), own, number, TOK_DEV, EXPERTS, TOP_K, CAP, 1))(expert_ids_keys, expert_ids_turns).reshape((TOKENS, TOP_K))
    gate_weights = jnp.clip(jnp.exp(math.log(1.0) - 2.3025851 * jax.random.uniform(own_keys[3], (TOKENS, TOP_K), jnp.float32) ** shard_levels(own_keys[3], (TOKENS, TOP_K), ((0, 16),), -0.2, 0.2)), 0.1, 1.0)
    expert_gate = gaussian(streams_of[4], (EXPERTS, D, FE), D ** -0.5, 0.125, ((0, 8), (2, 2)))
    expert_up = gaussian(streams_of[5], (EXPERTS, D, FE), D ** -0.5, 0.125, ((0, 8), (2, 2)))
    expert_down = gaussian(streams_of[6], (EXPERTS, FE, D), FE ** -0.5, 0.25, ((0, 8), (1, 2)))
    shared_gate = gaussian(streams_of[7], (D, FS), D ** -0.5, 0.125)
    shared_up = gaussian(streams_of[8], (D, FS), D ** -0.5, 0.125)
    shared_down = gaussian(streams_of[9], (FS, D), FS ** -0.5, 0.25)
    post_gain = jnp.clip(1.0 + 0.18 * jax.random.normal(streams_of[10], (D,), jnp.float32), 0.1, 1.9)
    return dict(tokens=tokens, norm_gain=norm_gain, expert_ids=expert_ids, gate_weights=gate_weights, expert_gate=expert_gate, expert_up=expert_up, expert_down=expert_down, shared_gate=shared_gate, shared_up=shared_up, shared_down=shared_down, post_gain=post_gain)


EPS = 1e-06

def rms_scale(inputs, gain):
    mean_sq = lax.optimization_barrier(jnp.mean(inputs * inputs, axis=-1, keepdims=True))
    return inputs * lax.rsqrt(mean_sq + EPS) * gain.astype(jnp.float32)

def swiglu_out(tok_rows, w_gate, w_up, w_down):
    gate_act = jnp.dot(tok_rows, w_gate, preferred_element_type=jnp.float32)
    up_act = jnp.dot(tok_rows, w_up, preferred_element_type=jnp.float32)
    hidden = (jax.nn.silu(gate_act) * up_act).astype(jnp.bfloat16)
    return jnp.dot(hidden, w_down, preferred_element_type=jnp.float32)

def reference(tokens, norm_gain, expert_ids, gate_weights, expert_gate, expert_up, expert_down, shared_gate, shared_up, shared_down, post_gain):
    tok_total = tokens.shape[0]
    width = tokens.shape[1]
    blocks = tok_total // TOK_DEV
    normed = rms_scale(tokens.astype(jnp.float32), norm_gain).astype(jnp.bfloat16)
    ids_blocked = expert_ids.reshape(blocks, TOK_DEV * TOP_K)
    onehot = (ids_blocked[:, :, None] == jnp.arange(EXPERTS, dtype=jnp.int32)[None, None, :]).astype(jnp.int32)
    slot_index = lax.optimization_barrier(jnp.sum(jnp.cumsum(onehot, axis=1) * onehot, axis=2)) - 1
    block_index = jnp.arange(blocks, dtype=jnp.int32)[:, None]
    position = (ids_blocked * (blocks * CAP) + block_index * CAP + slot_index).reshape(-1)
    source_row = (block_index * TOK_DEV + jnp.arange(TOK_DEV * TOP_K, dtype=jnp.int32)[None, :] // TOP_K).reshape(-1)
    lookup = jnp.full((EXPERTS * blocks * CAP,), tok_total, jnp.int32).at[position].set(source_row)
    lookup = lookup.reshape(EXPERTS, blocks * CAP)
    weight_table = jnp.zeros((EXPERTS * blocks * CAP,), jnp.float32).at[position].set(gate_weights.reshape(-1))
    weight_table = weight_table.reshape(EXPERTS, blocks * CAP)
    padded = jnp.concatenate([normed, jnp.zeros((1, width), jnp.bfloat16)], axis=0)

    def add_expert(combined, inputs):
        table_rows, table_weights, w_gate, w_up, w_down = inputs
        result = swiglu_out(padded[table_rows], w_gate, w_up, w_down).astype(jnp.bfloat16)
        combined = combined.at[table_rows].add(table_weights[:, None] * result.astype(jnp.float32))
        return (combined, None)
    start = jnp.zeros((tok_total + 1, width), jnp.float32)
    combined, _ = lax.scan(add_expert, start, (lookup, weight_table, expert_gate, expert_up, expert_down))
    shared_out = swiglu_out(normed, shared_gate, shared_up, shared_down)
    combined = combined[:tok_total] + shared_out
    return rms_scale(combined, post_gain).astype(jnp.bfloat16)
```

```python
import functools

import jax
import jax.numpy as jnp
from jax import lax
from jax.experimental import pallas as pl
from jax.experimental.pallas import tpu as pltpu
from jax.sharding import PartitionSpec as P

EXPERTS = 32
CAP = 40


EPS = 1e-06


def rms_scale(inputs, gain):
    mean_sq = jnp.mean(inputs * inputs, axis=-1, keepdims=True)
    return inputs * lax.rsqrt(mean_sq + EPS) * gain


def expert_rows(tok_rows, w_gate, w_up, w_down):
    gate_act = jnp.einsum("erd,edf->erf", tok_rows, w_gate, preferred_element_type=jnp.float32)
    up_act = jnp.einsum("erd,edf->erf", tok_rows, w_up, preferred_element_type=jnp.float32)
    hidden = (jax.nn.silu(gate_act) * up_act).astype(jnp.bfloat16)
    return jnp.einsum("erf,efd->erd", hidden, w_down, preferred_element_type=jnp.float32)


def shared_branch(normed, shared_gate, shared_up, shared_down):
    shared_act = jnp.dot(normed, shared_gate, preferred_element_type=jnp.float32)
    shared_lift = jnp.dot(normed, shared_up, preferred_element_type=jnp.float32)
    shared_hidden = (jax.nn.silu(shared_act) * shared_lift).astype(jnp.bfloat16)
    return jnp.dot(shared_hidden, shared_down, preferred_element_type=jnp.float32)


def body(
    tokens,
    norm_gain,
    expert_ids,
    gate_weights,
    expert_gate,
    expert_up,
    expert_down,
    shared_gate,
    shared_up,
    shared_down,
    post_gain,
):
    tok_count = tokens.shape[0]
    top_count = expert_ids.shape[1]
    width = tokens.shape[1]
    normed = rms_scale(tokens.astype(jnp.float32), norm_gain).astype(jnp.bfloat16)
    flat_ids = expert_ids.reshape(-1)
    onehot = (flat_ids[:, None] == jnp.arange(EXPERTS, dtype=jnp.int32)[None, :]).astype(jnp.int32)
    slot_index = jnp.sum(jnp.cumsum(onehot, axis=0) * onehot, axis=1) - 1
    position = flat_ids * CAP + slot_index
    source_row = jnp.arange(tok_count * top_count, dtype=jnp.int32) // top_count
    lookup = jnp.full((EXPERTS * CAP,), tok_count, jnp.int32).at[position].set(source_row)
    padded = jnp.concatenate([normed, jnp.zeros((1, width), jnp.bfloat16)], axis=0)
    outgoing = padded[lookup].reshape(EXPERTS, 1, CAP, width)
    whole_gate, whole_up, whole_down = (
        lax.all_gather(expert_gate, "tp", axis=2, tiled=True),
        lax.all_gather(expert_up, "tp", axis=2, tiled=True),
        lax.all_gather(expert_down, "tp", axis=1, tiled=True),
    )
    arrived = lax.all_to_all(outgoing, "ep", split_axis=0, concat_axis=1, tiled=True)
    local_experts = arrived.shape[0]
    senders = arrived.shape[1]
    slots = arrived.shape[2]
    tok_rows = arrived.reshape(local_experts, senders * slots, width)
    result = expert_rows(tok_rows, whole_gate, whole_up, whole_down).astype(jnp.bfloat16)
    result = result.reshape(local_experts, senders, slots, width)
    returned = lax.all_to_all(result, "ep", split_axis=1, concat_axis=0, tiled=True)
    shared_out = shared_branch(normed, shared_gate, shared_up, shared_down)
    back_rows = returned.reshape(EXPERTS * CAP, width)
    picked = back_rows[position].reshape(tok_count, top_count, width).astype(jnp.float32)
    routed = jnp.einsum("tk,tkd->td", gate_weights, picked)
    combined = routed + shared_out
    return rms_scale(combined, post_gain).astype(jnp.bfloat16)

VMEM_ALL = 67043328
MESH = pl.DeviceIdType.MESH
AHEAD = 2


def ring_place(ep, n):
    half, odd = ep // 2, ep % 2
    return half * (1 - odd) + (n - 1 - half) * odd


def ring_member(place, n):
    back = place // (n // 2)
    return 2 * place * (1 - back) + (2 * (n - 1 - place) + 1) * back


def kernel(
    n,
    top,
    tok_ref,
    meta_ref,
    ngain_ref,
    pgain_ref,
    eg_hbm,
    eu_hbm,
    ed_hbm,
    sg_hbm,
    su_hbm,
    sd_hbm,
    out_ref,
    wg,
    wu,
    wd,
    sg,
    su,
    sd,
    ag,
    meta,
    rs_in,
    rs_out,
    part,
    shared,
    hid,
    cols,
    load_sem,
    w_send,
    w_recv,
    ag_send,
    ag_recv,
    mt_send,
    mt_recv,
    rs_send,
    rs_recv,
):
    rows, width = tok_ref.shape
    experts = eg_hbm.shape[0]
    fh = eg_hbm.shape[2]
    half = rows // 2
    step_rows = 32
    ep = lax.axis_index("ep")
    tp = lax.axis_index("tp")
    me = ring_place(ep, n)
    right = ring_member((me + 1) % n, n)
    left = ring_member((me + n - 1) % n, n)
    partner = 1 - tp

    barrier = pltpu.get_barrier_semaphore()
    for where in ({"ep": right}, {"ep": left}, {"tp": partner}):
        pl.semaphore_signal(barrier, inc=1, device_id=where, device_id_type=MESH)

    loads = [
        pltpu.make_async_copy(src, dst, load_sem.at[k])
        for k, (src, dst) in enumerate(
            (
                (sg_hbm, sg),
                (su_hbm, su),
                (sd_hbm, sd),
                (eg_hbm, wg.at[0]),
                (eu_hbm, wu.at[0]),
                (ed_hbm, wd.at[0]),
            )
        )
    ]
    for load in loads:
        load.start()

    meta[0] = meta_ref[...]

    @pl.loop(0, rows // step_rows)
    def _(r):
        at = pl.ds(pl.multiple_of(r * step_rows, step_rows), step_rows)
        v = tok_ref[at, :].astype(jnp.float32)
        ag[0, at, :] = rms_scale(v, ngain_ref[...]).astype(jnp.bfloat16)

    pl.semaphore_wait(barrier, 3)

    def token_copy(way, s):
        lane = pl.ds(way * half, half)
        return pltpu.make_async_remote_copy(
            src_ref=ag.at[s, lane],
            dst_ref=ag.at[s + 1, lane],
            send_sem=ag_send.at[way, s],
            recv_sem=ag_recv.at[way, s + 1],
            device_id={"ep": (right, left)[way]},
            device_id_type=MESH,
        )

    def meta_copy(way, s):
        lane = pl.ds(way * half, half)
        return pltpu.make_async_remote_copy(
            src_ref=meta.at[s, :, lane],
            dst_ref=meta.at[s + 1, :, lane],
            send_sem=mt_send.at[way, s],
            recv_sem=mt_recv.at[way, s + 1],
            device_id={"ep": (right, left)[way]},
            device_id_type=MESH,
        )

    def sum_copy(way, s):
        lane = pl.ds(way * half, half)
        return pltpu.make_async_remote_copy(
            src_ref=rs_out.at[s % 2, lane],
            dst_ref=rs_in.at[s - 1, lane],
            send_sem=rs_send.at[way, s % 2],
            recv_sem=rs_recv.at[way, s - 1],
            device_id={"ep": (right, left)[way]},
            device_id_type=MESH,
        )

    for way in range(2):
        meta_copy(way, 0).start()
        token_copy(way, 0).start()

    swaps = [
        pltpu.make_async_remote_copy(
            src_ref=src,
            dst_ref=dst.at[1],
            send_sem=w_send.at[k],
            recv_sem=w_recv.at[k],
            device_id={"tp": partner},
            device_id_type=MESH,
        )
        for k, (src, dst) in enumerate(((eg_hbm, wg), (eu_hbm, wu), (ed_hbm, wd)))
    ]
    for swap in swaps:
        swap.start()

    def take(s):
        for way in range(2):
            meta_copy(way, s - 1).wait_recv()
            token_copy(way, s - 1).wait_recv()

            @pl.when(s < n - 1)
            def _():
                meta_copy(way, s).start()
                token_copy(way, s).start()

    for load in loads[:3]:
        load.wait()
    fs = sg.shape[1]
    for k in range(fs // fh):
        at = slice(k * fh, (k + 1) * fh)
        g = jnp.dot(ag[0], sg[:, at], preferred_element_type=jnp.float32)
        u = jnp.dot(ag[0], su[:, at], preferred_element_type=jnp.float32)
        hid[0, :, at] = (jax.nn.silu(g) * u).astype(jnp.bfloat16)

    tile = min(512, width)

    @pl.loop(0, width // tile)
    def _(j):
        at = pl.ds(pl.multiple_of(j * tile, tile), tile)
        shared[:, at] = jnp.dot(hid[0, :, :fs], sd[:, at], preferred_element_type=jnp.float32)

    for s in range(1, min(AHEAD, n - 1) + 1):
        take(s)
    for load in loads[3:]:
        load.wait()
    for swap in swaps:
        swap.wait_recv()

    def block(slot):
        table = meta[slot]
        lines = []
        for j in range(experts):
            number = (ep * experts + j).astype(jnp.float32)
            hit = jnp.where(table[:top] == number, table[top : 2 * top], 0.0)
            lines.append(jnp.sum(hit, axis=0, keepdims=True))
        lines.append(jnp.zeros((-experts % 8, rows), jnp.float32)) if experts % 8 else None
        turned = jnp.concatenate(lines, axis=0).T
        for j in range(experts):
            cols[j] = jnp.broadcast_to(turned[:, j : j + 1], (rows, 128))

        @pl.loop(0, experts)
        def _(e):
            scale = cols[e][:, :1]
            at = pl.ds(pl.multiple_of(e * fh, fh), fh)
            for h in range(2):
                g = jnp.dot(ag[slot], wg[h, e], preferred_element_type=jnp.float32)
                u = jnp.dot(ag[slot], wu[h, e], preferred_element_type=jnp.float32)
                hid[h, :, at] = (jax.nn.silu(g) * u * scale).astype(jnp.bfloat16)

        @pl.loop(0, width // tile)
        def _(j):
            at = pl.ds(pl.multiple_of(j * tile, tile), tile)
            total = jnp.zeros((rows, tile), jnp.float32)
            for h in range(2):
                down = wd[h, :, :, at].reshape(experts * fh, tile)
                total += jnp.dot(hid[h], down, preferred_element_type=jnp.float32)
            part[:, at] = total

    def each_rows(fn):
        @pl.loop(0, rows // step_rows)
        def _(r):
            fn(pl.ds(pl.multiple_of(r * step_rows, step_rows), step_rows))

    @pl.loop(1, n + 1)
    def _(s):
        block(s % n)

        @pl.when(s + AHEAD < n)
        def _():
            take(s + AHEAD)

        @pl.when(s > 1)
        def _():
            for way in range(2):
                sum_copy(way, s - 1).wait_recv()

        @pl.when(s < n)
        def _():
            @pl.when(s > 2)
            def _():
                for way in range(2):
                    sum_copy(way, s - 2).wait_send()

            @pl.when(s == 1)
            def _():
                def put(at):
                    rs_out[s % 2, at, :] = part[at, :].astype(jnp.bfloat16)

                each_rows(put)

            @pl.when(s > 1)
            def _():
                def put(at):
                    both = part[at, :] + rs_in[s - 2, at, :].astype(jnp.float32)
                    rs_out[s % 2, at, :] = both.astype(jnp.bfloat16)

                each_rows(put)

            for way in range(2):
                sum_copy(way, s).start()

    def finish(at):
        both = part[at, :] + rs_in[n - 2, at, :].astype(jnp.float32) + shared[at, :]
        out_ref[at, :] = rms_scale(both, pgain_ref[...]).astype(jnp.bfloat16)

    each_rows(finish)

    for swap in swaps:
        swap.wait_send()
    for way in range(2):
        for s in range(n - 1):
            meta_copy(way, s).wait_send()
            token_copy(way, s).wait_send()
        for s in range(max(1, n - 2), n):
            sum_copy(way, s).wait_send()


def ring_shapes(n, rows, width, meta_rows, eg, ed, sg, sd):
    bf, f32 = jnp.bfloat16, jnp.float32
    experts, _, fh = eg.shape
    fs = sg.shape[1]
    return [
        ((2,) + eg.shape, bf),
        ((2,) + eg.shape, bf),
        ((2,) + ed.shape, bf),
        (sg.shape, bf),
        (sg.shape, bf),
        (sd.shape, bf),
        ((n, rows, width), bf),
        ((n, meta_rows, rows), f32),
        ((n - 1, rows, width), bf),
        ((2, rows, width), bf),
        ((rows, width), f32),
        ((rows, width), f32),
        ((2, rows, max(experts * fh, fs)), bf),
        ((experts, rows, 128), f32),
    ]


def ring_bytes(shapes):
    total = 0
    for shape, kind in shapes:
        count = jnp.dtype(kind).itemsize
        for size in shape:
            count *= size
        total += count
    return total


def ring_body(
    n,
    tokens,
    norm_gain,
    expert_ids,
    gate_weights,
    expert_gate,
    expert_up,
    expert_down,
    shared_gate,
    shared_up,
    shared_down,
    post_gain,
):
    rows, width = tokens.shape
    top = expert_ids.shape[1]
    meta_rows = -(-2 * top // 8) * 8
    shapes = ring_shapes(n, rows, width, meta_rows, expert_gate, expert_down, shared_gate, shared_down)
    if ring_bytes(shapes) + 4 * rows * width > VMEM_ALL - (2 << 20):
        return body(
            tokens,
            norm_gain,
            expert_ids,
            gate_weights,
            expert_gate,
            expert_up,
            expert_down,
            shared_gate,
            shared_up,
            shared_down,
            post_gain,
        )
    meta = jnp.concatenate([expert_ids.T.astype(jnp.float32), gate_weights.T], axis=0)
    meta = jnp.pad(meta, ((0, meta_rows - 2 * top), (0, 0)))
    dma = pltpu.SemaphoreType.DMA
    vmem = pl.BlockSpec(memory_space=pltpu.VMEM)
    hbm = pl.BlockSpec(memory_space=pl.ANY)
    return pl.pallas_call(
        functools.partial(kernel, n, top),
        out_shape=jax.ShapeDtypeStruct((rows, width), jnp.bfloat16),
        in_specs=[vmem] * 4 + [hbm] * 6,
        out_specs=vmem,
        scratch_shapes=[pltpu.VMEM(shape, kind) for shape, kind in shapes]
        + [
            dma((6,)),
            dma((3,)),
            dma((3,)),
            dma((2, n)),
            dma((2, n)),
            dma((2, n)),
            dma((2, n)),
            dma((2, 2)),
            dma((2, n)),
        ],
        compiler_params=pltpu.CompilerParams(
            collective_id=0, has_side_effects=True, vmem_limit_bytes=VMEM_ALL
        ),
    )(
        tokens,
        meta,
        norm_gain.reshape(1, width),
        post_gain.reshape(1, width),
        expert_gate,
        expert_up,
        expert_down,
        shared_gate,
        shared_up,
        shared_down,
    )


def solution(mesh):
    ringed = mesh.shape["tp"] == 2 and mesh.shape["ep"] % 2 == 0 and mesh.shape["ep"] > 2
    return jax.shard_map(
        functools.partial(ring_body, mesh.shape["ep"]) if ringed else body,
        mesh=mesh,
        in_specs=(
            P(("grp", "ep", "tp"), None),
            P(),
            P(("grp", "ep", "tp"), None),
            P(("grp", "ep", "tp"), None),
            P("ep", None, "tp"),
            P("ep", None, "tp"),
            P("ep", "tp", None),
            P(),
            P(),
            P(),
            P(),
        ),
        out_specs=P(("grp", "ep", "tp"), None),
        check_vma=False,
    )
```

```python
import functools

import jax
import jax.numpy as jnp
from jax import lax
from jax.experimental import pallas as pl
from jax.experimental.pallas import tpu as pltpu
from jax.sharding import PartitionSpec as P

EXPERTS = 32
CAP = 40


EPS = 1e-06


def rms_scale(inputs, gain):
    mean_sq = jnp.mean(inputs * inputs, axis=-1, keepdims=True)
    return inputs * lax.rsqrt(mean_sq + EPS) * gain


def expert_rows(tok_rows, w_gate, w_up, w_down):
    gate_act = jnp.einsum("erd,edf->erf", tok_rows, w_gate, preferred_element_type=jnp.float32)
    up_act = jnp.einsum("erd,edf->erf", tok_rows, w_up, preferred_element_type=jnp.float32)
    hidden = (jax.nn.silu(gate_act) * up_act).astype(jnp.bfloat16)
    return jnp.einsum("erf,efd->erd", hidden, w_down, preferred_element_type=jnp.float32)


def shared_branch(normed, shared_gate, shared_up, shared_down):
    shared_act = jnp.dot(normed, shared_gate, preferred_element_type=jnp.float32)
    shared_lift = jnp.dot(normed, shared_up, preferred_element_type=jnp.float32)
    shared_hidden = (jax.nn.silu(shared_act) * shared_lift).astype(jnp.bfloat16)
    return jnp.dot(shared_hidden, shared_down, preferred_element_type=jnp.float32)


def body(
    tokens,
    norm_gain,
    expert_ids,
    gate_weights,
    expert_gate,
    expert_up,
    expert_down,
    shared_gate,
    shared_up,
    shared_down,
    post_gain,
):
    tok_count = tokens.shape[0]
    top_count = expert_ids.shape[1]
    width = tokens.shape[1]
    normed = rms_scale(tokens.astype(jnp.float32), norm_gain).astype(jnp.bfloat16)
    flat_ids = expert_ids.reshape(-1)
    onehot = (flat_ids[:, None] == jnp.arange(EXPERTS, dtype=jnp.int32)[None, :]).astype(jnp.int32)
    slot_index = jnp.sum(jnp.cumsum(onehot, axis=0) * onehot, axis=1) - 1
    position = flat_ids * CAP + slot_index
    source_row = jnp.arange(tok_count * top_count, dtype=jnp.int32) // top_count
    lookup = jnp.full((EXPERTS * CAP,), tok_count, jnp.int32).at[position].set(source_row)
    padded = jnp.concatenate([normed, jnp.zeros((1, width), jnp.bfloat16)], axis=0)
    outgoing = padded[lookup].reshape(EXPERTS, 1, CAP, width)
    whole_gate, whole_up, whole_down = (
        lax.all_gather(expert_gate, "tp", axis=2, tiled=True),
        lax.all_gather(expert_up, "tp", axis=2, tiled=True),
        lax.all_gather(expert_down, "tp", axis=1, tiled=True),
    )
    arrived = lax.all_to_all(outgoing, "ep", split_axis=0, concat_axis=1, tiled=True)
    local_experts = arrived.shape[0]
    senders = arrived.shape[1]
    slots = arrived.shape[2]
    tok_rows = arrived.reshape(local_experts, senders * slots, width)
    result = expert_rows(tok_rows, whole_gate, whole_up, whole_down).astype(jnp.bfloat16)
    result = result.reshape(local_experts, senders, slots, width)
    returned = lax.all_to_all(result, "ep", split_axis=1, concat_axis=0, tiled=True)
    shared_out = shared_branch(normed, shared_gate, shared_up, shared_down)
    back_rows = returned.reshape(EXPERTS * CAP, width)
    picked = back_rows[position].reshape(tok_count, top_count, width).astype(jnp.float32)
    routed = jnp.einsum("tk,tkd->td", gate_weights, picked)
    combined = routed + shared_out
    return rms_scale(combined, post_gain).astype(jnp.bfloat16)

VMEM_ALL = 67043328
MESH = pl.DeviceIdType.MESH


TAKE, SERVE, DENSE, MERGE, WAIT = range(5)
PLANS = {
    4: (
        ("T1", "W0", "S0", "D0", "S1", "T2", "D1", "M1", "S2", "T3", "D2", "M2", "S3", "D3", "M3", "M0"),
        ("T2", "T0", "W0", "S1", "D1", "S2", "T3", "S0", "D2", "S3", "D3", "M2", "D0", "M3", "M0", "M1"),
    ),
}


def is_equal(value, k, size):
    def at_least(low):
        return (value + size - low) // size if low < size else 0

    return at_least(k) - at_least(k + 1) if k > 0 else 1 - at_least(1)


def step_of(plan, z, i, size):
    mirror = z // (size // 2)
    near = z * (1 - mirror) + (size - 1 - z) * mirror
    words = plan
    count = len(words[0])
    kind, block = 0, 0
    for k in range(count):
        here = is_equal(i, k, count)
        for r in range(len(plan)):
            both = here * is_equal(near, r, len(plan))
            kind = kind + "TSDMW".index(words[r][k][0]) * both
            block = block + int(words[r][k][1]) * both
    return kind, block * (1 - mirror) + (size - 1 - block) * mirror


def kernel(
    size,
    top,
    tok_ref,
    meta_ref,
    ngain_ref,
    pgain_ref,
    eg_hbm,
    eu_hbm,
    ed_hbm,
    sg_hbm,
    su_hbm,
    sd_hbm,
    out_ref,
    wg,
    wu,
    wd,
    sg,
    su,
    sd,
    ag,
    meta,
    y_out,
    y_in,
    yr_in,
    rs_in,
    rs_out,
    stage,
    hid,
    cols,
    tri,
    load_sem,
    w_send,
    w_recv,
    ag_send,
    ag_recv,
    mt_send,
    mt_recv,
    yd_send,
    yd_recv,
    yr_send,
    yr_recv,
    rs_send,
    rs_recv,
):
    rows, width = tok_ref.shape
    experts = eg_hbm.shape[0]
    fh = eg_hbm.shape[2]
    slots = experts * CAP
    step_rows = 32
    tile = min(512, width)
    pieces = width // tile
    last = size - 1
    bf, f32 = jnp.bfloat16, jnp.float32
    ep = lax.axis_index("ep")
    z, y = ep // 2, ep % 2
    pair = z * 2 + 1 - y
    partner = 1 - lax.axis_index("tp")
    plan = PLANS[size]

    barrier = pltpu.get_barrier_semaphore()

    def greet(where):
        pl.semaphore_signal(barrier, inc=1, device_id=where, device_id_type=MESH)

    @pl.when(z < last)
    def _():
        greet({"ep": (z + 1) * 2 + y})

    @pl.when(z > 0)
    def _():
        greet({"ep": (z - 1) * 2 + y})

    greet({"ep": pair})
    greet({"tp": partner})

    loads = [
        pltpu.make_async_copy(src, dst, load_sem.at[k])
        for k, (src, dst) in enumerate(
            (
                (sg_hbm, sg),
                (su_hbm, su),
                (sd_hbm, sd),
                (eg_hbm, wg.at[0]),
                (eu_hbm, wu.at[0]),
                (ed_hbm, wd.at[0]),
            )
        )
    ]
    for load in loads:
        load.start()

    meta[z] = meta_ref[...]
    before = lax.broadcasted_iota(jnp.int32, (rows, rows), 0) < lax.broadcasted_iota(jnp.int32, (rows, rows), 1)
    tri[...] = jnp.where(before, 1.0, 0.0).astype(bf)

    @pl.loop(0, rows // step_rows)
    def _(r):
        at = pl.ds(pl.multiple_of(r * step_rows, step_rows), step_rows)
        v = tok_ref[at, :].astype(f32)
        ag[z, at, :] = rms_scale(v, ngain_ref[...]).astype(bf)

    pl.semaphore_wait(barrier, 2 + (z + last) // size + (last - z + last) // size)

    def piece(q):
        return pl.ds(q * tile, tile)

    def remote(src, dst, send, recv, where):
        return pltpu.make_async_remote_copy(
            src_ref=src, dst_ref=dst, send_sem=send, recv_sem=recv, device_id=where, device_id_type=MESH
        )

    def token_copy(b, q, zt, slot):
        ref = ag.at[b, :, piece(q)]
        return remote(ref, ref, ag_send.at[slot, q], ag_recv.at[b, q], {"ep": zt * 2 + y})

    def meta_copy(b, zt, slot):
        return remote(meta.at[b], meta.at[b], mt_send.at[slot], mt_recv.at[b], {"ep": zt * 2 + y})

    def row_copy(b, q):
        at = piece(q)
        return remote(y_out.at[b, :, at], y_in.at[b, :, at], yd_send.at[b, q], yd_recv.at[b, q], {"ep": pair})

    def back_copy(b, q):
        at = piece(q)
        return remote(y_in.at[b, :, at], yr_in.at[b, :, at], yr_send.at[b, q], yr_recv.at[b, q], {"ep": pair})

    def sum_copy(b, q, zt, slot):
        at = piece(q)
        return remote(
            rs_out.at[b, :, at], rs_in.at[slot, :, at], rs_send.at[b, q], rs_recv.at[slot, q], {"ep": zt * 2 + y}
        )

    def own_sends(act):
        @pl.when(z < last)
        def _():
            act(meta_copy(z, z + 1, z))

        @pl.when(z > 0)
        def _():
            act(meta_copy(z, z - 1, size))

        for q in range(pieces):

            @pl.when(z < last)
            def _():
                act(token_copy(z, q, z + 1, z))

            @pl.when(z > 0)
            def _():
                act(token_copy(z, q, z - 1, size))

    own_sends(lambda copy: copy.start())

    def onward(b, fn):
        @pl.when((b < z) & (z < last))
        def _():
            fn(z + 1)

        @pl.when((b > z) & (z > 0))
        def _():
            fn(z - 1)

    def targets(b, number_of):
        seen = meta[b]
        hits, weights = [], []
        for j in range(experts):
            number = (number_of * experts + j).astype(f32)
            same = seen[:top] == number
            hits.append(jnp.sum(jnp.where(same, 1.0, 0.0), axis=0, keepdims=True))
            weights.append(jnp.sum(jnp.where(same, seen[top : 2 * top], 0.0), axis=0, keepdims=True))
        blank = -experts % 8
        if blank:
            hits.append(jnp.zeros((blank, rows), f32))
            weights.append(jnp.zeros((blank, rows), f32))
        return jnp.concatenate(hits, axis=0), jnp.concatenate(weights, axis=0)

    def places(hits):
        rank = jnp.dot(hits.astype(bf), tri[...], preferred_element_type=f32)
        first = lax.broadcasted_iota(jnp.int32, hits.shape, 0).astype(f32) * CAP
        return jnp.where(hits > 0.0, rank + first, -1.0)

    def dispatch(b):
        hits, _ = targets(b, pair)
        spot = places(hits)
        line = lax.broadcasted_iota(jnp.int32, (slots, rows), 0).astype(f32)
        pick = jnp.zeros((slots, rows), f32)
        for j in range(experts):
            pick = jnp.where(line == spot[j : j + 1], 1.0, pick)
        pick = pick.astype(bf)
        for q in range(pieces):
            at = piece(q)
            y_out[b, :, at] = jnp.dot(pick, ag[b, :, at], preferred_element_type=f32).astype(bf)
            row_copy(b, q).start()

    def take(b):
        meta_copy(b, z, z).wait_recv()
        onward(b, lambda zt: meta_copy(b, zt, b).start())
        for q in range(pieces):
            token_copy(b, q, z, z).wait_recv()
            onward(b, lambda zt: token_copy(b, q, zt, b).start())
        dispatch(b)

    def hidden_of(x_ref, scale_of, count):
        @pl.loop(0, experts)
        def _(e):
            scale = scale_of(e)
            at = pl.ds(pl.multiple_of(e * fh, fh), fh)
            for h in range(2):
                g = jnp.dot(x_ref[...], wg[h, e], preferred_element_type=f32)
                u = jnp.dot(x_ref[...], wu[h, e], preferred_element_type=f32)
                hid[h, :count, at] = (jax.nn.silu(g) * u * scale).astype(bf)

    def down_of(count, q):
        total = jnp.zeros((count, tile), f32)
        for h in range(2):
            down = wd[h, :, :, piece(q)].reshape(experts * fh, tile)
            total += jnp.dot(hid[h, :count, : experts * fh], down, preferred_element_type=f32)
        return total

    def serve(b):
        for q in range(pieces):
            row_copy(b, q).wait_recv()
        line = lax.broadcasted_iota(jnp.int32, (slots, fh), 0)
        hidden_of(
            y_in.at[b],
            lambda e: jnp.where((line >= e * CAP) & (line < (e + 1) * CAP), 1.0, 0.0),
            slots,
        )
        for q in range(pieces):
            y_in[b, :, piece(q)] = down_of(slots, q).astype(bf)
            back_copy(b, q).start()

    def place_of(b):
        apart = ((b - z) * (b - z) + size * size - 1) // (size * size)
        return 2 - apart * (2 - b % 2)

    def dense(b):
        _, weights = targets(b, ep)
        turned = weights.T
        for j in range(experts):
            cols[j] = jnp.broadcast_to(turned[:, j : j + 1], (rows, 128))
        hidden_of(ag.at[b], lambda e: cols[e][:, :1], rows)
        for q in range(pieces):
            total = down_of(rows, q)

            @pl.when(b == z)
            def _():
                stage[2, :, piece(q)] += total

            @pl.when(b != z)
            def _():
                stage[b % 2, :, piece(q)] = total

    def merge(b):
        hits, weights = targets(b, pair)
        spot = places(hits).T
        turned = weights.T
        lane = lax.broadcasted_iota(jnp.int32, (rows, slots), 1).astype(f32)
        mix = jnp.zeros((rows, slots), f32)
        for j in range(experts):
            mix = jnp.where(lane == spot[:, j : j + 1], turned[:, j : j + 1], mix)
        high = mix.astype(bf)
        low = (mix - high.astype(f32)).astype(bf)
        own = b == z
        here = place_of(b)

        for q in range(pieces):
            at = piece(q)
            back_copy(b, q).wait_recv()
            came = yr_in[b, :, at]
            stage[here, :, at] += jnp.dot(high, came, preferred_element_type=f32) + jnp.dot(
                low, came, preferred_element_type=f32
            )

            @pl.when(((b >= z) & (z > 0)) | ((b < z) & (z < last)))
            def _():
                sum_copy(b, q, z, b).wait_recv()
                stage[here, :, at] += rs_in[b, :, at].astype(f32)

            @pl.when(own & (z < last))
            def _():
                sum_copy(b, q, z, size).wait_recv()
                stage[here, :, at] += rs_in[size, :, at].astype(f32)

            @pl.when(jnp.logical_not(own))
            def _():
                rs_out[b, :, at] = stage[here, :, at].astype(bf)

            @pl.when(b > z)
            def _():
                sum_copy(b, q, z + 1, b).start()

            @pl.when(b < z - 1)
            def _():
                sum_copy(b, q, z - 1, b).start()

            @pl.when(b == z - 1)
            def _():
                sum_copy(b, q, z - 1, size).start()

    swaps = [
        remote(src, dst.at[1], w_send.at[k], w_recv.at[k], {"tp": partner})
        for k, (src, dst) in enumerate(((eg_hbm, wg), (eu_hbm, wu), (ed_hbm, wd)))
    ]
    dispatch(z)
    for swap in swaps:
        swap.start()

    for load in loads[:3]:
        load.wait()
    fs = sg.shape[1]
    for k in range(fs // fh):
        at = slice(k * fh, (k + 1) * fh)
        g = jnp.dot(ag[z], sg[:, at], preferred_element_type=f32)
        u = jnp.dot(ag[z], su[:, at], preferred_element_type=f32)
        hid[0, :, at] = (jax.nn.silu(g) * u).astype(bf)

    @pl.loop(0, pieces)
    def _(j):
        at = pl.ds(pl.multiple_of(j * tile, tile), tile)
        stage[2, :, at] = jnp.dot(hid[0, :, :fs], sd[:, at], preferred_element_type=f32)

    def weights_in(b):
        for load in loads[3:]:
            load.wait()
        for swap in swaps:
            swap.wait_recv()

    @pl.loop(0, len(plan[0]))
    def _(i):
        kind, b = step_of(plan, z, i, size)
        for number, fn in ((TAKE, take), (SERVE, serve), (DENSE, dense), (MERGE, merge), (WAIT, weights_in)):

            @pl.when(kind == number)
            def _():
                fn(b)

    @pl.loop(0, rows // step_rows)
    def _(r):
        at = pl.ds(pl.multiple_of(r * step_rows, step_rows), step_rows)
        out_ref[at, :] = rms_scale(stage[2, at, :], pgain_ref[...]).astype(bf)

    for swap in swaps:
        swap.wait_send()
    own_sends(lambda copy: copy.wait_send())

    @pl.loop(0, size)
    def _(b):
        onward(b, lambda zt: meta_copy(b, zt, b).wait_send())
        for q in range(pieces):
            onward(b, lambda zt: token_copy(b, q, zt, b).wait_send())
            row_copy(b, q).wait_send()
            back_copy(b, q).wait_send()

            @pl.when(b > z)
            def _():
                sum_copy(b, q, z, b).wait_send()

            @pl.when(b < z)
            def _():
                sum_copy(b, q, z, b).wait_send()


def ring_shapes(n, rows, width, meta_rows, eg, ed, sg, sd):
    bf, f32 = jnp.bfloat16, jnp.float32
    experts, _, fh = eg.shape
    fs = sg.shape[1]
    size = n // 2
    slots = experts * CAP
    return [
        ((2,) + eg.shape, bf),
        ((2,) + eg.shape, bf),
        ((2,) + ed.shape, bf),
        (sg.shape, bf),
        (sg.shape, bf),
        (sd.shape, bf),
        ((size, rows, width), bf),
        ((size, meta_rows, rows), f32),
        ((size, slots, width), bf),
        ((size, slots, width), bf),
        ((size, slots, width), bf),
        ((size + 1, rows, width), bf),
        ((size, rows, width), bf),
        ((3, rows, width), f32),
        ((2, rows, max(experts * fh, fs)), bf),
        ((experts, rows, 128), f32),
        ((rows, rows), bf),
    ]


def ring_bytes(shapes):
    total = 0
    for shape, kind in shapes:
        count = jnp.dtype(kind).itemsize
        for size in shape:
            count *= size
        total += count
    return total


def ring_body(
    n,
    tokens,
    norm_gain,
    expert_ids,
    gate_weights,
    expert_gate,
    expert_up,
    expert_down,
    shared_gate,
    shared_up,
    shared_down,
    post_gain,
):
    rows, width = tokens.shape
    top = expert_ids.shape[1]
    meta_rows = -(-2 * top // 8) * 8
    shapes = ring_shapes(n, rows, width, meta_rows, expert_gate, expert_down, shared_gate, shared_down)
    if ring_bytes(shapes) + 4 * rows * width > VMEM_ALL - (2 << 20):
        return body(
            tokens,
            norm_gain,
            expert_ids,
            gate_weights,
            expert_gate,
            expert_up,
            expert_down,
            shared_gate,
            shared_up,
            shared_down,
            post_gain,
        )
    meta = jnp.concatenate([expert_ids.T.astype(jnp.float32), gate_weights.T], axis=0)
    meta = jnp.pad(meta, ((0, meta_rows - 2 * top), (0, 0)))
    dma = pltpu.SemaphoreType.DMA
    size = n // 2
    pieces = width // min(512, width)
    vmem = pl.BlockSpec(memory_space=pltpu.VMEM)
    hbm = pl.BlockSpec(memory_space=pl.ANY)
    return pl.pallas_call(
        functools.partial(kernel, size, top),
        out_shape=jax.ShapeDtypeStruct((rows, width), jnp.bfloat16),
        in_specs=[vmem] * 4 + [hbm] * 6,
        out_specs=vmem,
        scratch_shapes=[pltpu.VMEM(shape, kind) for shape, kind in shapes]
        + [
            dma((6,)),
            dma((3,)),
            dma((3,)),
            dma((size + 1, pieces)),
            dma((size, pieces)),
            dma((size + 1,)),
            dma((size,)),
            dma((size, pieces)),
            dma((size, pieces)),
            dma((size, pieces)),
            dma((size, pieces)),
            dma((size, pieces)),
            dma((size + 1, pieces)),
        ],
        compiler_params=pltpu.CompilerParams(
            collective_id=0, has_side_effects=True, vmem_limit_bytes=VMEM_ALL
        ),
    )(
        tokens,
        meta,
        norm_gain.reshape(1, width),
        post_gain.reshape(1, width),
        expert_gate,
        expert_up,
        expert_down,
        shared_gate,
        shared_up,
        shared_down,
    )


def solution(mesh):
    ringed = mesh.shape["tp"] == 2 and mesh.shape["ep"] % 2 == 0 and mesh.shape["ep"] // 2 in PLANS
    return jax.shard_map(
        functools.partial(ring_body, mesh.shape["ep"]) if ringed else body,
        mesh=mesh,
        in_specs=(
            P(("grp", "ep", "tp"), None),
            P(),
            P(("grp", "ep", "tp"), None),
            P(("grp", "ep", "tp"), None),
            P("ep", None, "tp"),
            P("ep", None, "tp"),
            P("ep", "tp", None),
            P(),
            P(),
            P(),
            P(),
        ),
        out_specs=P(("grp", "ep", "tp"), None),
        check_vma=False,
    )
```

```python
import functools

import jax
import jax.numpy as jnp
from jax import lax
from jax.experimental import pallas as pl
from jax.experimental.pallas import tpu as pltpu
from jax.sharding import PartitionSpec as P

EXPERTS = 32
CAP = 40


EPS = 1e-06


def rms_scale(inputs, gain):
    mean_sq = jnp.mean(inputs * inputs, axis=-1, keepdims=True)
    return inputs * lax.rsqrt(mean_sq + EPS) * gain


def expert_rows(tok_rows, w_gate, w_up, w_down):
    gate_act = jnp.einsum("erd,edf->erf", tok_rows, w_gate, preferred_element_type=jnp.float32)
    up_act = jnp.einsum("erd,edf->erf", tok_rows, w_up, preferred_element_type=jnp.float32)
    hidden = (jax.nn.silu(gate_act) * up_act).astype(jnp.bfloat16)
    return jnp.einsum("erf,efd->erd", hidden, w_down, preferred_element_type=jnp.float32)


def shared_branch(normed, shared_gate, shared_up, shared_down):
    shared_act = jnp.dot(normed, shared_gate, preferred_element_type=jnp.float32)
    shared_lift = jnp.dot(normed, shared_up, preferred_element_type=jnp.float32)
    shared_hidden = (jax.nn.silu(shared_act) * shared_lift).astype(jnp.bfloat16)
    return jnp.dot(shared_hidden, shared_down, preferred_element_type=jnp.float32)


def body(
    tokens,
    norm_gain,
    expert_ids,
    gate_weights,
    expert_gate,
    expert_up,
    expert_down,
    shared_gate,
    shared_up,
    shared_down,
    post_gain,
):
    tok_count = tokens.shape[0]
    top_count = expert_ids.shape[1]
    width = tokens.shape[1]
    normed = rms_scale(tokens.astype(jnp.float32), norm_gain).astype(jnp.bfloat16)
    flat_ids = expert_ids.reshape(-1)
    onehot = (flat_ids[:, None] == jnp.arange(EXPERTS, dtype=jnp.int32)[None, :]).astype(jnp.int32)
    slot_index = jnp.sum(jnp.cumsum(onehot, axis=0) * onehot, axis=1) - 1
    position = flat_ids * CAP + slot_index
    source_row = jnp.arange(tok_count * top_count, dtype=jnp.int32) // top_count
    lookup = jnp.full((EXPERTS * CAP,), tok_count, jnp.int32).at[position].set(source_row)
    padded = jnp.concatenate([normed, jnp.zeros((1, width), jnp.bfloat16)], axis=0)
    outgoing = padded[lookup].reshape(EXPERTS, 1, CAP, width)
    whole_gate, whole_up, whole_down = (
        lax.all_gather(expert_gate, "tp", axis=2, tiled=True),
        lax.all_gather(expert_up, "tp", axis=2, tiled=True),
        lax.all_gather(expert_down, "tp", axis=1, tiled=True),
    )
    arrived = lax.all_to_all(outgoing, "ep", split_axis=0, concat_axis=1, tiled=True)
    local_experts = arrived.shape[0]
    senders = arrived.shape[1]
    slots = arrived.shape[2]
    tok_rows = arrived.reshape(local_experts, senders * slots, width)
    result = expert_rows(tok_rows, whole_gate, whole_up, whole_down).astype(jnp.bfloat16)
    result = result.reshape(local_experts, senders, slots, width)
    returned = lax.all_to_all(result, "ep", split_axis=1, concat_axis=0, tiled=True)
    shared_out = shared_branch(normed, shared_gate, shared_up, shared_down)
    back_rows = returned.reshape(EXPERTS * CAP, width)
    picked = back_rows[position].reshape(tok_count, top_count, width).astype(jnp.float32)
    routed = jnp.einsum("tk,tkd->td", gate_weights, picked)
    combined = routed + shared_out
    return rms_scale(combined, post_gain).astype(jnp.bfloat16)

VMEM_ALL = 67043328
MESH = pl.DeviceIdType.MESH


TAKE, SERVE, DENSE, MERGE, WAIT = range(5)
PLANS = {
    4: (
        ("T1", "W0", "S0", "D0", "T2", "D2", "T3", "D3", "S3", "S2", "S1", "M3", "D1", "M2", "M1", "M0"),
        ("T2", "T0", "W0", "D1", "T3", "S1", "D3", "S3", "S0", "D0", "S2", "M3", "M0", "D2", "M2", "M1"),
    ),
}


def is_equal(value, k, size):
    def at_least(low):
        return (value + size - low) // size if low < size else 0

    return at_least(k) - at_least(k + 1) if k > 0 else 1 - at_least(1)


def step_of(plan, z, i, size):
    mirror = z // (size // 2)
    near = z * (1 - mirror) + (size - 1 - z) * mirror
    words = plan
    count = len(words[0])
    kind, block = 0, 0
    for k in range(count):
        here = is_equal(i, k, count)
        for r in range(len(plan)):
            both = here * is_equal(near, r, len(plan))
            kind = kind + "TSDMW".index(words[r][k][0]) * both
            block = block + int(words[r][k][1]) * both
    return kind, block * (1 - mirror) + (size - 1 - block) * mirror


def kernel(
    size,
    top,
    tok_ref,
    meta_ref,
    ngain_ref,
    pgain_ref,
    eg_hbm,
    eu_hbm,
    ed_hbm,
    sg_hbm,
    su_hbm,
    sd_hbm,
    out_ref,
    wg,
    wu,
    wd,
    sg,
    su,
    sd,
    ag,
    meta,
    y_out,
    y_in,
    yr_in,
    rs_in,
    rs_out,
    stage,
    hid,
    cols,
    tri,
    load_sem,
    w_send,
    w_recv,
    ag_send,
    ag_recv,
    mt_send,
    mt_recv,
    yd_send,
    yd_recv,
    yr_send,
    yr_recv,
    rs_send,
    rs_recv,
):
    rows, width = tok_ref.shape
    experts = eg_hbm.shape[0]
    fh = eg_hbm.shape[2]
    slots = experts * CAP
    step_rows = 32
    tile = min(512, width)
    pieces = width // tile
    last = size - 1
    bf, f32 = jnp.bfloat16, jnp.float32
    ep = lax.axis_index("ep")
    z, y = ep // 2, ep % 2
    pair = z * 2 + 1 - y
    partner = 1 - lax.axis_index("tp")
    plan = PLANS[size]

    barrier = pltpu.get_barrier_semaphore()

    def greet(where):
        pl.semaphore_signal(barrier, inc=1, device_id=where, device_id_type=MESH)

    @pl.when(z < last)
    def _():
        greet({"ep": (z + 1) * 2 + y})

    @pl.when(z > 0)
    def _():
        greet({"ep": (z - 1) * 2 + y})

    greet({"ep": pair})
    greet({"tp": partner})

    loads = [
        pltpu.make_async_copy(src, dst, load_sem.at[k])
        for k, (src, dst) in enumerate(
            (
                (sg_hbm, sg),
                (su_hbm, su),
                (sd_hbm, sd),
                (eg_hbm, wg.at[0]),
                (eu_hbm, wu.at[0]),
                (ed_hbm, wd.at[0]),
            )
        )
    ]
    for load in loads:
        load.start()

    meta[z] = meta_ref[...]
    before = lax.broadcasted_iota(jnp.int32, (rows, rows), 0) < lax.broadcasted_iota(jnp.int32, (rows, rows), 1)
    tri[...] = jnp.where(before, 1.0, 0.0).astype(bf)

    @pl.loop(0, rows // step_rows)
    def _(r):
        at = pl.ds(pl.multiple_of(r * step_rows, step_rows), step_rows)
        v = tok_ref[at, :].astype(f32)
        ag[z, at, :] = rms_scale(v, ngain_ref[...]).astype(bf)

    pl.semaphore_wait(barrier, 2 + (z + last) // size + (last - z + last) // size)

    def piece(q):
        return pl.ds(q * tile, tile)

    def remote(src, dst, send, recv, where):
        return pltpu.make_async_remote_copy(
            src_ref=src, dst_ref=dst, send_sem=send, recv_sem=recv, device_id=where, device_id_type=MESH
        )

    def token_copy(b, q, zt, slot):
        ref = ag.at[b, :, piece(q)]
        return remote(ref, ref, ag_send.at[slot, q], ag_recv.at[b, q], {"ep": zt * 2 + y})

    def meta_copy(b, zt, slot):
        return remote(meta.at[b], meta.at[b], mt_send.at[slot], mt_recv.at[b], {"ep": zt * 2 + y})

    def row_copy(b, q):
        at = piece(q)
        return remote(y_out.at[b, :, at], y_in.at[b, :, at], yd_send.at[b, q], yd_recv.at[b, q], {"ep": pair})

    def back_copy(b, q):
        at = piece(q)
        return remote(y_in.at[b, :, at], yr_in.at[b, :, at], yr_send.at[b, q], yr_recv.at[b, q], {"ep": pair})

    def sum_copy(b, q, zt, slot):
        at = piece(q)
        return remote(
            rs_out.at[b, :, at], rs_in.at[slot, :, at], rs_send.at[b, q], rs_recv.at[slot, q], {"ep": zt * 2 + y}
        )

    def own_sends(act):
        @pl.when(z < last)
        def _():
            act(meta_copy(z, z + 1, z))

        @pl.when(z > 0)
        def _():
            act(meta_copy(z, z - 1, size))

        for q in range(pieces):

            @pl.when(z < last)
            def _():
                act(token_copy(z, q, z + 1, z))

            @pl.when(z > 0)
            def _():
                act(token_copy(z, q, z - 1, size))

    own_sends(lambda copy: copy.start())

    def onward(b, fn):
        @pl.when((b < z) & (z < last))
        def _():
            fn(z + 1)

        @pl.when((b > z) & (z > 0))
        def _():
            fn(z - 1)

    def targets(b, number_of):
        seen = meta[b]
        hits, weights = [], []
        for j in range(experts):
            number = (number_of * experts + j).astype(f32)
            same = seen[:top] == number
            hits.append(jnp.sum(jnp.where(same, 1.0, 0.0), axis=0, keepdims=True))
            weights.append(jnp.sum(jnp.where(same, seen[top : 2 * top], 0.0), axis=0, keepdims=True))
        blank = -experts % 8
        if blank:
            hits.append(jnp.zeros((blank, rows), f32))
            weights.append(jnp.zeros((blank, rows), f32))
        return jnp.concatenate(hits, axis=0), jnp.concatenate(weights, axis=0)

    def places(hits):
        rank = jnp.dot(hits.astype(bf), tri[...], preferred_element_type=f32)
        first = lax.broadcasted_iota(jnp.int32, hits.shape, 0).astype(f32) * CAP
        return jnp.where(hits > 0.0, rank + first, -1.0)

    def dispatch(b):
        hits, _ = targets(b, pair)
        spot = places(hits)
        line = lax.broadcasted_iota(jnp.int32, (slots, rows), 0).astype(f32)
        pick = jnp.zeros((slots, rows), f32)
        for j in range(experts):
            pick = jnp.where(line == spot[j : j + 1], 1.0, pick)
        pick = pick.astype(bf)
        for q in range(pieces):
            at = piece(q)
            y_out[b, :, at] = jnp.dot(pick, ag[b, :, at], preferred_element_type=f32).astype(bf)
            row_copy(b, q).start()

    def take(b):
        meta_copy(b, z, z).wait_recv()
        onward(b, lambda zt: meta_copy(b, zt, b).start())
        for q in range(pieces):
            token_copy(b, q, z, z).wait_recv()
            onward(b, lambda zt: token_copy(b, q, zt, b).start())
        dispatch(b)

    def hidden_of(x_ref, scale_of, count):
        @pl.loop(0, experts)
        def _(e):
            scale = scale_of(e)
            at = pl.ds(pl.multiple_of(e * fh, fh), fh)
            for h in range(2):
                g = jnp.dot(x_ref[...], wg[h, e], preferred_element_type=f32)
                u = jnp.dot(x_ref[...], wu[h, e], preferred_element_type=f32)
                hid[h, :count, at] = (jax.nn.silu(g) * u * scale).astype(bf)

    def down_of(count, q):
        total = jnp.zeros((count, tile), f32)
        for h in range(2):
            down = wd[h, :, :, piece(q)].reshape(experts * fh, tile)
            total += jnp.dot(hid[h, :count, : experts * fh], down, preferred_element_type=f32)
        return total

    def serve(b):
        for q in range(pieces):
            row_copy(b, q).wait_recv()
        line = lax.broadcasted_iota(jnp.int32, (slots, fh), 0)
        hidden_of(
            y_in.at[b],
            lambda e: jnp.where((line >= e * CAP) & (line < (e + 1) * CAP), 1.0, 0.0),
            slots,
        )
        for q in range(pieces):
            y_in[b, :, piece(q)] = down_of(slots, q).astype(bf)
            back_copy(b, q).start()

    def place_of(b):
        apart = ((b - z) * (b - z) + size * size - 1) // (size * size)
        return 2 - apart * (2 - b % 2)

    def dense(b):
        _, weights = targets(b, ep)
        turned = weights.T
        for j in range(experts):
            cols[j] = jnp.broadcast_to(turned[:, j : j + 1], (rows, 128))
        hidden_of(ag.at[b], lambda e: cols[e][:, :1], rows)
        for q in range(pieces):
            total = down_of(rows, q)

            @pl.when(b == z)
            def _():
                stage[2, :, piece(q)] += total

            @pl.when(b != z)
            def _():
                stage[b % 2, :, piece(q)] = total

    def merge(b):
        hits, weights = targets(b, pair)
        spot = places(hits).T
        turned = weights.T
        lane = lax.broadcasted_iota(jnp.int32, (rows, slots), 1).astype(f32)
        mix = jnp.zeros((rows, slots), f32)
        for j in range(experts):
            mix = jnp.where(lane == spot[:, j : j + 1], turned[:, j : j + 1], mix)
        high = mix.astype(bf)
        low = (mix - high.astype(f32)).astype(bf)
        own = b == z
        here = place_of(b)

        for q in range(pieces):
            at = piece(q)
            back_copy(b, q).wait_recv()
            came = yr_in[b, :, at]
            stage[here, :, at] += jnp.dot(high, came, preferred_element_type=f32) + jnp.dot(
                low, came, preferred_element_type=f32
            )

            @pl.when(((b >= z) & (z > 0)) | ((b < z) & (z < last)))
            def _():
                sum_copy(b, q, z, b).wait_recv()
                stage[here, :, at] += rs_in[b, :, at].astype(f32)

            @pl.when(own & (z < last))
            def _():
                sum_copy(b, q, z, size).wait_recv()
                stage[here, :, at] += rs_in[size, :, at].astype(f32)

            @pl.when(jnp.logical_not(own))
            def _():
                rs_out[b, :, at] = stage[here, :, at].astype(bf)

            @pl.when(b > z)
            def _():
                sum_copy(b, q, z + 1, b).start()

            @pl.when(b < z - 1)
            def _():
                sum_copy(b, q, z - 1, b).start()

            @pl.when(b == z - 1)
            def _():
                sum_copy(b, q, z - 1, size).start()

    swaps = [
        remote(src, dst.at[1], w_send.at[k], w_recv.at[k], {"tp": partner})
        for k, (src, dst) in enumerate(((eg_hbm, wg), (eu_hbm, wu), (ed_hbm, wd)))
    ]
    dispatch(z)
    for swap in swaps:
        swap.start()

    for load in loads[:3]:
        load.wait()
    fs = sg.shape[1]
    for k in range(fs // fh):
        at = slice(k * fh, (k + 1) * fh)
        g = jnp.dot(ag[z], sg[:, at], preferred_element_type=f32)
        u = jnp.dot(ag[z], su[:, at], preferred_element_type=f32)
        hid[0, :, at] = (jax.nn.silu(g) * u).astype(bf)

    @pl.loop(0, pieces)
    def _(j):
        at = pl.ds(pl.multiple_of(j * tile, tile), tile)
        stage[2, :, at] = jnp.dot(hid[0, :, :fs], sd[:, at], preferred_element_type=f32)

    def weights_in(b):
        for load in loads[3:]:
            load.wait()
        for swap in swaps:
            swap.wait_recv()

    @pl.loop(0, len(plan[0]))
    def _(i):
        kind, b = step_of(plan, z, i, size)
        for number, fn in ((TAKE, take), (SERVE, serve), (DENSE, dense), (MERGE, merge), (WAIT, weights_in)):

            @pl.when(kind == number)
            def _():
                fn(b)

    @pl.loop(0, rows // step_rows)
    def _(r):
        at = pl.ds(pl.multiple_of(r * step_rows, step_rows), step_rows)
        out_ref[at, :] = rms_scale(stage[2, at, :], pgain_ref[...]).astype(bf)

    for swap in swaps:
        swap.wait_send()
    own_sends(lambda copy: copy.wait_send())

    @pl.loop(0, size)
    def _(b):
        onward(b, lambda zt: meta_copy(b, zt, b).wait_send())
        for q in range(pieces):
            onward(b, lambda zt: token_copy(b, q, zt, b).wait_send())
            row_copy(b, q).wait_send()
            back_copy(b, q).wait_send()

            @pl.when(b > z)
            def _():
                sum_copy(b, q, z, b).wait_send()

            @pl.when(b < z)
            def _():
                sum_copy(b, q, z, b).wait_send()


def ring_shapes(n, rows, width, meta_rows, eg, ed, sg, sd):
    bf, f32 = jnp.bfloat16, jnp.float32
    experts, _, fh = eg.shape
    fs = sg.shape[1]
    size = n // 2
    slots = experts * CAP
    return [
        ((2,) + eg.shape, bf),
        ((2,) + eg.shape, bf),
        ((2,) + ed.shape, bf),
        (sg.shape, bf),
        (sg.shape, bf),
        (sd.shape, bf),
        ((size, rows, width), bf),
        ((size, meta_rows, rows), f32),
        ((size, slots, width), bf),
        ((size, slots, width), bf),
        ((size, slots, width), bf),
        ((size + 1, rows, width), bf),
        ((size, rows, width), bf),
        ((3, rows, width), f32),
        ((2, rows, max(experts * fh, fs)), bf),
        ((experts, rows, 128), f32),
        ((rows, rows), bf),
    ]


def ring_bytes(shapes):
    total = 0
    for shape, kind in shapes:
        count = jnp.dtype(kind).itemsize
        for size in shape:
            count *= size
        total += count
    return total


def ring_body(
    n,
    tokens,
    norm_gain,
    expert_ids,
    gate_weights,
    expert_gate,
    expert_up,
    expert_down,
    shared_gate,
    shared_up,
    shared_down,
    post_gain,
):
    rows, width = tokens.shape
    top = expert_ids.shape[1]
    meta_rows = -(-2 * top // 8) * 8
    shapes = ring_shapes(n, rows, width, meta_rows, expert_gate, expert_down, shared_gate, shared_down)
    if ring_bytes(shapes) + 4 * rows * width > VMEM_ALL - (2 << 20):
        return body(
            tokens,
            norm_gain,
            expert_ids,
            gate_weights,
            expert_gate,
            expert_up,
            expert_down,
            shared_gate,
            shared_up,
            shared_down,
            post_gain,
        )
    meta = jnp.concatenate([expert_ids.T.astype(jnp.float32), gate_weights.T], axis=0)
    meta = jnp.pad(meta, ((0, meta_rows - 2 * top), (0, 0)))
    dma = pltpu.SemaphoreType.DMA
    size = n // 2
    pieces = width // min(512, width)
    vmem = pl.BlockSpec(memory_space=pltpu.VMEM)
    hbm = pl.BlockSpec(memory_space=pl.ANY)
    return pl.pallas_call(
        functools.partial(kernel, size, top),
        out_shape=jax.ShapeDtypeStruct((rows, width), jnp.bfloat16),
        in_specs=[vmem] * 4 + [hbm] * 6,
        out_specs=vmem,
        scratch_shapes=[pltpu.VMEM(shape, kind) for shape, kind in shapes]
        + [
            dma((6,)),
            dma((3,)),
            dma((3,)),
            dma((size + 1, pieces)),
            dma((size, pieces)),
            dma((size + 1,)),
            dma((size,)),
            dma((size, pieces)),
            dma((size, pieces)),
            dma((size, pieces)),
            dma((size, pieces)),
            dma((size, pieces)),
            dma((size + 1, pieces)),
        ],
        compiler_params=pltpu.CompilerParams(
            collective_id=0, has_side_effects=True, vmem_limit_bytes=VMEM_ALL
        ),
    )(
        tokens,
        meta,
        norm_gain.reshape(1, width),
        post_gain.reshape(1, width),
        expert_gate,
        expert_up,
        expert_down,
        shared_gate,
        shared_up,
        shared_down,
    )


def solution(mesh):
    ringed = mesh.shape["tp"] == 2 and mesh.shape["ep"] % 2 == 0 and mesh.shape["ep"] // 2 in PLANS
    return jax.shard_map(
        functools.partial(ring_body, mesh.shape["ep"]) if ringed else body,
        mesh=mesh,
        in_specs=(
            P(("grp", "ep", "tp"), None),
            P(),
            P(("grp", "ep", "tp"), None),
            P(("grp", "ep", "tp"), None),
            P("ep", None, "tp"),
            P("ep", None, "tp"),
            P("ep", "tp", None),
            P(),
            P(),
            P(),
            P(),
        ),
        out_specs=P(("grp", "ep", "tp"), None),
        check_vma=False,
    )
```
